256 devices in a mesh: grp: 2 (over y), sp: 16 (over z), tp: 4 (over x), dp: 2 (over core).
Axes of the slice: x: 4, y: 2, z: 16, core: 2. Of those that a mesh axis runs over, the one named last changes fastest.
The devices are a block of a 4x16x16 slice.
Arguments:
- latent: bfloat16 [4, 6144, 2048], P(('grp', 'dp'), ('sp', 'tp')), parts along dimension 0, may hold values from -6 to 6
- cond: bfloat16 [4, 2048], P(('grp', 'dp')), parts along dimension 0, may hold values from -6 to 6
- context: bfloat16 [4, 256, 2048], P(('grp', 'dp'), 'sp'), parts along dimension 0, may hold values from -6 to 6
- cond_ctx: bfloat16 [2048], replicated, may hold values from -8 to 8
- w_shift: bfloat16 [2048, 2048], P('sp', 'tp'), may hold values from -0.125 to 0.125
- w_scale: bfloat16 [2048, 2048], P('sp', 'tp'), may hold values from -0.125 to 0.125
- w_gate: bfloat16 [2048, 2048], P('sp', 'tp'), may hold values from -0.125 to 0.125
- norm_gain: float32 [2048], replicated, may hold values from 0.1 to 1.9
- w_query: bfloat16 [2048, 1024], P(None, 'tp'), may hold values from -0.125 to 0.125
- w_key: bfloat16 [2048, 512], P(None, 'tp'), may hold values from -0.125 to 0.125
- w_value: bfloat16 [2048, 512], P(None, 'tp'), may hold values from -0.125 to 0.125
- query_gain: float32 [128], replicated, may hold values from 0.6 to 16
- key_gain: float32 [128], replicated, may hold values from 0.6 to 16
- ctx_lift: float32 [8], P('tp'), may hold values from -2 to 0.5
- out_gain: float32 [1024], replicated, may hold values from 0.1 to 1.9
- w_out: bfloat16 [1024, 2048], replicated, may hold values from -0.1875 to 0.1875
Outputs:
- result: bfloat16 [4, 6144, 2048], P(('grp', 'dp'), ('sp', 'tp')), parts along dimension 0
The draws below stay inside these ranges and needn't reach their ends.
There are 2 independent parts, one for each index of `grp`. The reference program is written for one: setup_inputs(seed, part) draws one part's arguments, and reference() takes and returns one part's arrays. A program takes and returns all parts, laid end to end along the dimension named above; an argument that names none is the same for every part. Nothing has to cross between parts.
All inputs are finite; a program needn't handle non-finite values.
Results may differ from the reference program's by a relative error of at most 0.023.
The reference program's roundings to bfloat16 on the way count: a program that leaves them out, or rounds other values in their place, can miss the bound.
Values may be sent and summed in bfloat16 or wider, within the bound.
No kernel may reach another device: no remote copies, remote signals or barrier semaphores. Data moves between devices by JAX's collectives and lax.ppermute only.
A program may use at most 64 MiB of HBM per device.

```python
import math
import jax
import jax.numpy as jnp
from jax import lax

D = 2048
HEADS = 8
KV_HEADS = 4
HEAD_DIM = 128
GRID_WIDTH = 64
TOK_DEV = 384
CONTEXT = 256
BATCH = 2
TOKENS = 6144
N_SP = 16


def gain_common(key, role):
    logs = jax.random.uniform(jax.random.fold_in(key, role), (HEAD_DIM,), jnp.float32, jnp.log(0.6), jnp.log(2.2))
    base = jnp.exp(logs)
    return base


def draw_query_gain(key, part):
    return gain_common(key, 11)


def draw_key_gain(key, part):
    return gain_common(key, 12)


def level_of(own_key, extent, pieces, low, top_value):
    level, own = 1.0, jax.random.fold_in(own_key, 6)
    for dim, shards_of in pieces:
        heights = jnp.exp(jax.random.uniform(jax.random.fold_in(own, dim), (shards_of,), jnp.float32, low / len(pieces), top_value / len(pieces)))
        level = level * jnp.repeat(heights, extent[dim] // shards_of).reshape([-1 if axis == dim else 1 for axis in range(len(extent))])
    return level


def noise(stream_key, extent, scale, limit, cuts=(), kind=jnp.bfloat16):
    drawn = scale * jax.random.normal(stream_key, extent, jnp.float32)
    if cuts:
        drawn = drawn * level_of(stream_key, extent, cuts, -0.22, 0.18)
    return jnp.clip(drawn, -limit, limit).astype(kind)


def setup_inputs(seed: int = 0, part: int = 0) -> dict:
    keys = jax.random.split(jax.random.key(seed), 17)
    own_keys = jax.random.split(jax.random.fold_in(keys[16], part), 17)
    latent = noise(own_keys[0], (BATCH, TOKENS, D), 1.0, 6.0, ((0, 2), (1, 64)))
    cond = noise(own_keys[1], (BATCH, D), 1.0, 6.0, ((0, 2),))
    context = noise(own_keys[2], (BATCH, CONTEXT, D), 1.0, 6.0, ((0, 2), (1, 16)))
    cond_ctx = noise(keys[3], (D,), 2.0, 8.0)
    w_shift = noise(keys[4], (D, D), D ** -0.5, 0.125, ((0, 16), (1, 4)))
    w_scale = noise(keys[5], (D, D), D ** -0.5, 0.125, ((0, 16), (1, 4)))
    w_gate = noise(keys[6], (D, D), D ** -0.5, 0.125, ((0, 16), (1, 4)))
    norm_gain = jnp.clip(1.0 + 0.18 * jax.random.normal(keys[7], (D,), jnp.float32), 0.1, 1.9)
    w_query = noise(keys[8], (D, HEADS * HEAD_DIM), D ** -0.5, 0.125, ((1, 4),))
    w_key = noise(keys[9], (D, KV_HEADS * HEAD_DIM), D ** -0.5, 0.125, ((1, 4),))
    w_value = noise(keys[10], (D, KV_HEADS * HEAD_DIM), D ** -0.5, 0.125, ((1, 4),))
    query_gain = draw_query_gain(jax.random.fold_in(keys[16], 71), part)
    key_gain = draw_key_gain(jax.random.fold_in(keys[16], 71), part)
    ctx_lift = jnp.clip(-2.0 + 2.5 * jax.random.uniform(keys[13], (HEADS,), jnp.float32) ** level_of(keys[13], (HEADS,), ((0, 4),), -0.2, 0.2), -2.0, 0.5)
    out_gain = jnp.clip(1.0 + 0.18 * jax.random.normal(keys[14], (HEADS * HEAD_DIM,), jnp.float32), 0.1, 1.9)
    w_out = noise(keys[15], (HEADS * HEAD_DIM, D), (HEADS * HEAD_DIM) ** -0.5, 0.1875)
    return dict(latent=latent, cond=cond, context=context, cond_ctx=cond_ctx, w_shift=w_shift, w_scale=w_scale, w_gate=w_gate, norm_gain=norm_gain, w_query=w_query, w_key=w_key, w_value=w_value, query_gain=query_gain, key_gain=key_gain, ctx_lift=ctx_lift, out_gain=out_gain, w_out=w_out)


EPSILON = 1e-06

def rotate(vectors, positions):
    freqs = vectors.shape[-1] // 4
    grid_rows = (positions // GRID_WIDTH).astype(jnp.float32)
    grid_cols = (positions % GRID_WIDTH).astype(jnp.float32)
    inverse = 10000.0 ** (-jnp.arange(freqs, dtype=jnp.float32) / freqs)
    angles = jnp.stack([grid_rows[:, None] * inverse, grid_cols[:, None] * inverse], axis=1)
    cosine = jnp.cos(angles)[:, None]
    sine = jnp.sin(angles)[:, None]
    split = vectors.reshape(vectors.shape[:-1] + (2, 2, freqs))
    first = split[..., 0, :]
    second = split[..., 1, :]
    return jnp.stack([first * cosine - second * sine, second * cosine + first * sine], axis=-2).reshape(vectors.shape)

def head_norm(vectors, gain_vector):
    floats = vectors.astype(jnp.float32)
    return floats * lax.rsqrt(lax.optimization_barrier(jnp.mean(floats * floats, -1, keepdims=True)) + EPSILON) * gain_vector.astype(jnp.float32)

def modulated_norm(row_data, gain_vector, shift_row, scale_row):
    floats = row_data.astype(jnp.float32)
    normal = floats * lax.rsqrt(lax.optimization_barrier(jnp.mean(floats * floats, -1, keepdims=True)) + EPSILON)
    return (normal * gain_vector * (1.0 + scale_row) + shift_row).astype(jnp.bfloat16)

def reference(latent, cond, context, cond_ctx, w_shift, w_scale, w_gate, norm_gain, w_query, w_key, w_value, query_gain, key_gain, ctx_lift, out_gain, w_out):
    group = HEADS // KV_HEADS
    inputs = jax.nn.silu(jnp.concatenate([cond, cond_ctx[None]], 0).astype(jnp.float32)).astype(jnp.bfloat16)
    shift_all = jnp.dot(inputs, w_shift, preferred_element_type=jnp.float32)
    scale_all = jnp.dot(inputs, w_scale, preferred_element_type=jnp.float32)
    gate_all = jnp.dot(inputs, w_gate, preferred_element_type=jnp.float32)
    batch = latent.shape[0]
    positions = jnp.arange(TOKENS, dtype=jnp.int32)
    lift_table = (ctx_lift + math.log(TOKENS / CONTEXT)).reshape(KV_HEADS, group)
    factor = HEAD_DIM ** (-0.5)
    outputs = []
    for sample in range(batch):
        normed = modulated_norm(latent[sample], norm_gain, shift_all[sample], scale_all[sample])
        query_rows = jnp.dot(normed, w_query, preferred_element_type=jnp.float32).astype(jnp.bfloat16)
        key_rows = jnp.dot(normed, w_key, preferred_element_type=jnp.float32).astype(jnp.bfloat16)
        value_rows = jnp.dot(normed, w_value, preferred_element_type=jnp.float32).astype(jnp.bfloat16)
        query_rows = rotate(head_norm(query_rows.reshape(TOKENS, HEADS, HEAD_DIM), query_gain), positions).astype(jnp.bfloat16)
        query_rows = query_rows.reshape(TOKENS, KV_HEADS, group, HEAD_DIM)
        key_rows = rotate(head_norm(key_rows.reshape(TOKENS, KV_HEADS, HEAD_DIM), key_gain), positions).astype(jnp.bfloat16)
        value_rows = value_rows.reshape(TOKENS, KV_HEADS, HEAD_DIM)
        ctx_normed = modulated_norm(context[sample], norm_gain, shift_all[batch], scale_all[batch])
        ctx_key_rows = jnp.dot(ctx_normed, w_key, preferred_element_type=jnp.float32).astype(jnp.bfloat16)
        ctx_key_rows = head_norm(ctx_key_rows.reshape(CONTEXT, KV_HEADS, HEAD_DIM), key_gain).astype(jnp.bfloat16)
        ctx_value_rows = jnp.dot(ctx_normed, w_value, preferred_element_type=jnp.float32).astype(jnp.bfloat16)
        ctx_value_rows = ctx_value_rows.reshape(CONTEXT, KV_HEADS, HEAD_DIM)
        key_float = key_rows.astype(jnp.float32)
        value_float = value_rows.astype(jnp.float32)
        ctx_key_float = ctx_key_rows.astype(jnp.float32)
        ctx_value_float = ctx_value_rows.astype(jnp.float32)

        def attend(block_queries):
            query_float = block_queries.astype(jnp.float32)
            latent_scores = jnp.einsum('qkgd,nkd->kgqn', query_float, key_float) * factor
            ctx_scores = jnp.einsum('qkgd,nkd->kgqn', query_float, ctx_key_float) * factor + lift_table[:, :, None, None]
            highest = jnp.maximum(lax.optimization_barrier(jnp.max(latent_scores, -1)), lax.optimization_barrier(jnp.max(ctx_scores, -1)))[..., None]
            latent_exp = jnp.exp(latent_scores - highest)
            ctx_exp = jnp.exp(ctx_scores - highest)
            denominator = lax.optimization_barrier(jnp.sum(latent_exp, -1)) + lax.optimization_barrier(jnp.sum(ctx_exp, -1))
            latent_weights = latent_exp.astype(jnp.bfloat16).astype(jnp.float32)
            ctx_weights = ctx_exp.astype(jnp.bfloat16).astype(jnp.float32)
            summed = jnp.einsum('kgqn,nkd->qkgd', latent_weights, value_float) + jnp.einsum('kgqn,nkd->qkgd', ctx_weights, ctx_value_float)
            return (summed / jnp.transpose(denominator, (2, 0, 1))[..., None]).astype(jnp.bfloat16)
        blocks = query_rows.reshape(N_SP, TOK_DEV, KV_HEADS, group, HEAD_DIM)
        attended = lax.map(attend, blocks).reshape(TOKENS, HEADS * HEAD_DIM)
        att_normed = head_norm(attended, out_gain).astype(jnp.bfloat16)
        mixture = jnp.dot(att_normed, w_out, preferred_element_type=jnp.float32)
        outputs.append((latent[sample].astype(jnp.float32) + gate_all[sample] * mixture).astype(jnp.bfloat16))
    return jnp.stack(outputs)
```

```python
import functools
import math

import jax
import jax.numpy as jnp
from jax import lax
from jax.experimental import pallas as pl
from jax.experimental.pallas import tpu as pltpu
from jax.sharding import PartitionSpec as P


HEADS = 8
HEAD_DIM = 128
GRID_WIDTH = 64
EPSILON = 1e-06
FACTOR = HEAD_DIM ** (-0.5)
LOG2E = math.log2(math.e)
F32 = jnp.float32
BF16 = jnp.bfloat16
MIB = 1 << 20


def local_call(body, outs, *, flops, limit=12, scratch=(), aliases=None):
    single = not isinstance(outs, (tuple, list))
    shapes = [outs] if single else list(outs)
    space = pl.BlockSpec(memory_space=pltpu.VMEM)

    def run(*args):
        moved = sum(a.size * a.dtype.itemsize for a in args)
        moved += sum(math.prod(o.shape) * o.dtype.itemsize for o in shapes)
        return pl.pallas_call(
            body,
            out_shape=outs if single else tuple(shapes),
            in_specs=[space] * len(args),
            out_specs=space if single else tuple([space] * len(shapes)),
            scratch_shapes=list(scratch),
            input_output_aliases=aliases or {},
            compiler_params=pltpu.CompilerParams(vmem_limit_bytes=limit * MIB),
            cost_estimate=pl.CostEstimate(
                flops=flops, bytes_accessed=moved, transcendentals=0
            ),
        )(*args)

    return run


FAR = pl.BlockSpec(memory_space=pltpu.MemorySpace.HBM)


def far(x):
    return pltpu.with_memory_space_constraint(x, pltpu.MemorySpace.HBM)


def shape(dims, dtype):
    return jax.ShapeDtypeStruct(dims, dtype)


def modulation_kernel(cond, cond_ctx, wa, wb, wc, out_ref, weights, sem):
    copies = [
        pltpu.make_async_copy(w, weights.at[i], sem.at[i]) for i, w in enumerate((wa, wb, wc))
    ]
    for copy in copies:
        copy.start()
    depth = weights.shape[1]
    at = pl.ds(pl.multiple_of(lax.axis_index("sp") * depth, depth), depth)
    rows = jnp.concatenate([cond[:, at].astype(F32), cond_ctx[:, at].astype(F32)], 0)
    acted = (rows * jax.nn.sigmoid(rows)).astype(BF16)
    for copy in copies:
        copy.wait()
    shift, scale, gate = (
        jnp.dot(acted, weights[i], preferred_element_type=F32) for i in range(3)
    )
    mod = jnp.concatenate([shift[0:1], scale[0:1], shift[1:2], scale[1:2]], 0)
    part = gate.shape[1] // 4
    gate = jnp.concatenate([gate[0:1, i * part : (i + 1) * part] for i in range(4)], 0)
    mod = jnp.concatenate([mod, gate], 1)
    for i in range(out_ref.shape[0]):
        out_ref[i] = mod


def sum_kernel(parts, out_ref):
    total = jnp.sum(parts[...], 0)
    for i in range(out_ref.shape[0]):
        out_ref[i] = total


def kv_kernel(
    x0, x1, x2, x3, ctx, mod, gain, wkv, key_gain, cosine, sine, chunk_ref, normed_ref
):
    wide = gain.shape[1] // mod.shape[0]

    def row_of(index):
        return jnp.concatenate([mod[b, index : index + 1, :wide] for b in range(mod.shape[0])], 1)

    gains = gain[...]
    amp, shift = gains * (1.0 + row_of(1)), row_of(0)

    def norm(rows, amp, shift):
        rows = rows.astype(F32)
        mean = jnp.mean(rows * rows, -1, keepdims=True)
        return (rows * lax.rsqrt(mean + EPSILON) * amp + shift).astype(BF16)

    ctx_rows = ctx.shape[0]
    normed_ref[0:ctx_rows, :] = norm(ctx[...], gains * (1.0 + row_of(3)), row_of(2))
    own = x0.shape[0]
    for block, x in enumerate((x0, x1, x2, x3)):
        for t in range(own // 16):
            at = ctx_rows + block * own + t * 16
            normed_ref[at : at + 16, :] = norm(x[t * 16 : t * 16 + 16, :], amp, shift)
    kv = jnp.dot(normed_ref[...], wkv[...], preferred_element_type=F32)
    chunk_ref[1] = kv[:, HEAD_DIM:].astype(BF16)
    k = head_norm(kv[:, :HEAD_DIM], key_gain[...])
    chunk_ref[0, 0:ctx_rows, :] = k[0:ctx_rows].astype(BF16)
    chunk_ref[0, ctx_rows:, :] = rotate(k[ctx_rows:], cosine[...], sine[...]).astype(BF16)


def head_norm(vectors, gain):
    floats = vectors.astype(BF16).astype(F32)
    return floats * lax.rsqrt(jnp.mean(floats * floats, -1, keepdims=True) + EPSILON) * gain


def rotate(vectors, cosine, signed_sine):
    lanes = vectors.shape[-1]
    quarter = lanes // 4
    lane = lax.broadcasted_iota(jnp.int32, vectors.shape, 1)
    up = pltpu.roll(vectors, lanes - quarter, 1)
    down = pltpu.roll(vectors, quarter, 1)
    partner = jnp.where(lane % (2 * quarter) < quarter, up, down)
    return vectors * cosine + partner * signed_sine


def query_kernel(normed, wq, query_gain, cosine, sine, out_ref):
    rows = cosine.shape[0]
    skip = normed.shape[0] - rows
    q = jnp.dot(normed[skip:, :], wq[...], preferred_element_type=F32)
    for h in range(q.shape[1] // HEAD_DIM):
        one = head_norm(q[:, h * HEAD_DIM : (h + 1) * HEAD_DIM], query_gain[...])
        one = rotate(one, cosine[...], sine[...])
        out_ref[:, h * rows : (h + 1) * rows] = one.T.astype(BF16)


def attend_kernel(ctx_rows, first, pairs, *refs):
    refs = list(refs)
    qt, lift = refs[0], refs[1]
    if pairs:
        chunks = [(refs[2], refs[3])]
        rest = refs[4:]
    else:
        count = len(refs) - 2 - (2 if first else 4)
        chunks = [(r.at[0], r.at[1]) for r in refs[2 : 2 + count]]
        rest = refs[2 + count :]
    if first:
        acc_out, stat_out = rest
    else:
        acc_in, stat_in, acc_out, stat_out = rest
    total = qt.shape[1]
    width = 256
    for begin in range(0, total, width):
        part = slice(begin, begin + width)
        q = qt[:, part]
        bias = lift[:, part]
        if first:
            top = low = acc = None
        else:
            top, low, acc = stat_in[0:1, part], stat_in[1:2, part], acc_in[:, part]
        for k_ref, v_ref in chunks:
            s = jnp.dot(k_ref[...], q, preferred_element_type=F32)
            s = jnp.concatenate([s[:ctx_rows] + bias, s[ctx_rows:]], 0)
            new = jnp.max(s, 0, keepdims=True)
            if top is not None:
                new = jnp.maximum(top, new)
            p = jnp.exp2((s - new) * (FACTOR * LOG2E))
            size = jnp.sum(p, 0, keepdims=True)
            mixed = lax.dot_general(
                v_ref[...], p.astype(BF16), (((0,), (0,)), ((), ())), preferred_element_type=F32
            )
            if top is None:
                low, acc = size, mixed
            else:
                keep = jnp.exp2((top - new) * (FACTOR * LOG2E))
                low, acc = low * keep + size, acc * keep + mixed
            top = new
        acc_out[:, part] = acc
        stat_out[0:1, part] = top
        stat_out[1:2, part] = low


def finish_kernel(acc, stat, *targets):
    own = targets[0].shape[0]
    rows = len(targets) * own
    for h in range(acc.shape[1] // rows):
        part = slice(h * rows, (h + 1) * rows)
        att = (acc[:, part] / stat[1:2, part]).T.astype(BF16)
        for b, target in enumerate(targets):
            target[:, h * HEAD_DIM : (h + 1) * HEAD_DIM] = att[b * own : (b + 1) * own]


def out_kernel(order, a0, a1, a2, a3, gain, w_out, latent, mod, out_ref, weights, sem):
    blocks = mod.shape[0]
    wide = out_ref.shape[1] // blocks
    copies = [
        pltpu.make_async_copy(w_out.at[:, pl.ds(b * wide, wide)], weights.at[b], sem.at[b])
        for b in range(blocks)
    ]
    for copy in copies:
        copy.start()
    cols = a0.shape[1]
    atts = [a[...].astype(F32) for a in (a0, a1, a2, a3)]
    total = sum(jnp.sum(a * a, -1, keepdims=True) for a in atts)
    scale = lax.rsqrt(total / (cols * len(atts)) + EPSILON)
    normed = [
        (a * scale * gain[pl.ds(order[i], 1), :]).astype(BF16) for i, a in enumerate(atts)
    ]
    for b in range(blocks):
        copies[b].wait()
        part = slice(b * wide, (b + 1) * wide)
        mix = 0.0
        for i, a in enumerate(normed):
            at = pl.multiple_of(order[i] * cols, cols)
            mix += jnp.dot(a, weights[b, pl.ds(at, cols), :], preferred_element_type=F32)
        gate = jnp.concatenate([mod[b, r : r + 1, wide:] for r in range(mod.shape[1])], 1)
        out = latent[:, part].astype(F32) + gate * mix
        out_ref[:, part] = out.astype(BF16)


def angles(positions):
    freqs = HEAD_DIM // 4
    rows = (positions // GRID_WIDTH).astype(F32)
    cols = (positions % GRID_WIDTH).astype(F32)
    inverse = 10000.0 ** (-jnp.arange(freqs, dtype=F32) / freqs)
    by_row, by_col = rows[:, None] * inverse, cols[:, None] * inverse
    cosine = [jnp.cos(by_row)] * 2 + [jnp.cos(by_col)] * 2
    sine = [-jnp.sin(by_row), jnp.sin(by_row), -jnp.sin(by_col), jnp.sin(by_col)]
    return jnp.concatenate(cosine, 1), jnp.concatenate(sine, 1)


def shifted(x, axis, by):
    count = lax.axis_size(axis)
    return lax.ppermute(x, axis, [(i, (i + by) % count) for i in range(count)])


def on_device(
    latent,
    cond,
    context,
    cond_ctx,
    w_shift,
    w_scale,
    w_gate,
    norm_gain,
    w_query,
    w_key,
    w_value,
    query_gain,
    key_gain,
    ctx_lift,
    out_gain,
    w_out,
):
    sp, tp = lax.axis_index("sp"), lax.axis_index("tp")
    n_sp, n_tp = lax.axis_size("sp"), lax.axis_size("tp")
    own_rows, width = latent.shape[1:]
    latent, context = latent[0], context[0]
    ctx_rows = context.shape[0]
    rows = own_rows * n_tp
    in_rows, out_cols = w_shift.shape

    space = pl.BlockSpec(memory_space=pltpu.VMEM)
    packed = (4, out_cols + out_cols // 4)
    parts = pl.pallas_call(
        modulation_kernel,
        out_shape=shape((n_sp, *packed), F32),
        in_specs=[space, space, FAR, FAR, FAR],
        out_specs=space,
        scratch_shapes=[
            pltpu.VMEM((3, in_rows, out_cols), BF16),
            pltpu.SemaphoreType.DMA((3,)),
        ],
        compiler_params=pltpu.CompilerParams(vmem_limit_bytes=4 * MIB),
        cost_estimate=pl.CostEstimate(flops=10**6, bytes_accessed=MIB, transcendentals=0),
        name="modulation",
    )(cond, cond_ctx[None], far(w_shift), far(w_scale), far(w_gate))
    parts = lax.all_to_all(parts, "sp", 0, 0)
    mod = local_call(sum_kernel, shape((n_tp, *packed), F32), flops=10**6, limit=4)(parts)
    mod = lax.all_to_all(mod, "tp", 0, 0)

    latents = [latent]
    for by in (1, -1, 2):
        latents.append(shifted(latent, "tp", by))
    owners = jnp.stack([tp, (tp - 1) % n_tp, (tp + 1) % n_tp, (tp + 2) % n_tp])
    positions = sp * rows + (owners[:, None] * own_rows + jnp.arange(own_rows)[None]).reshape(-1)
    cosine, sine = angles(positions.astype(jnp.int32))
    wkv = jnp.concatenate([w_key, w_value], 1)
    length = ctx_rows + rows
    chunk, normed = local_call(
        kv_kernel,
        (shape((2, length, HEAD_DIM), BF16), shape((length, width), BF16)),
        flops=2 * length * width * 256,
        limit=16,
    )(*latents, context, mod, norm_gain[None], wkv, key_gain[None], cosine, sine)
    q_cols = w_query.shape[1]
    group = q_cols // HEAD_DIM
    qt = local_call(
        query_kernel, shape((HEAD_DIM, group * rows), BF16), flops=2 * rows * width * q_cols, limit=16
    )(normed, w_query, query_gain[None], cosine, sine)
    lift = (ctx_lift + math.log(rows / ctx_rows)) / FACTOR
    lift = jnp.repeat(lift, rows)[None]

    lanes = group * rows
    state_shapes = (shape((HEAD_DIM, lanes), F32), shape((2, lanes), F32))
    state = local_call(
        functools.partial(attend_kernel, ctx_rows, True, False),
        state_shapes,
        flops=4 * length * lanes * HEAD_DIM,
    )(qt, lift, chunk)

    def attend(state, *chunks, pairs=False):
        count = 1 if pairs else len(chunks)
        given = (qt, lift, *chunks, *state)
        return local_call(
            functools.partial(attend_kernel, ctx_rows, False, pairs),
            state_shapes,
            flops=4 * count * length * lanes * HEAD_DIM,
            aliases={len(given) - 2: 0, len(given) - 1: 1},
        )(*given)

    right, left = shifted(chunk, "sp", 1), shifted(chunk, "sp", -1)
    for _ in range(n_sp // 2 - 2):
        right, left, state = lax.optimization_barrier((right, left, state))
        arrived = right, left
        right, left = shifted(right, "sp", 1), shifted(left, "sp", -1)
        state = attend(state, *arrived)
    right, left, state = lax.optimization_barrier((right, left, state))
    last_k, last_v = shifted(right[0], "sp", 1), shifted(left[1], "sp", -1)
    state = attend(state, right, left)
    state = attend(state, last_k, last_v, pairs=True)

    own, to_left, to_right, to_far = local_call(
        finish_kernel, [shape((own_rows, q_cols), BF16)] * n_tp, flops=10**6
    )(*state)
    atts = [own, shifted(to_left, "tp", -1), shifted(to_right, "tp", 1), shifted(to_far, "tp", 2)]
    order = jnp.stack([tp, (tp + 1) % n_tp, (tp - 1) % n_tp, (tp + 2) % n_tp]).astype(jnp.int32)
    result = pl.pallas_call(
        out_kernel,
        out_shape=shape((own_rows, width), BF16),
        in_specs=[pl.BlockSpec(memory_space=pltpu.SMEM)] + [space] * 5 + [FAR, space, space],
        out_specs=space,
        scratch_shapes=[
            pltpu.VMEM((n_tp, w_out.shape[0], out_cols), BF16),
            pltpu.SemaphoreType.DMA((n_tp,)),
        ],
        compiler_params=pltpu.CompilerParams(vmem_limit_bytes=12 * MIB),
        cost_estimate=pl.CostEstimate(
            flops=2 * own_rows * width * HEADS * HEAD_DIM, bytes_accessed=5 * MIB, transcendentals=0
        ),
        name="output",
    )(order, *atts, out_gain.reshape(n_tp, q_cols), far(w_out), latent, mod)
    return result[None]


def solution(mesh):
    in_specs = (
        P(("grp", "dp"), ("sp", "tp"), None),
        P(("grp", "dp"), None),
        P(("grp", "dp"), "sp", None),
        P(),
        P("sp", "tp"),
        P("sp", "tp"),
        P("sp", "tp"),
        P(),
        P(None, "tp"),
        P(None, "tp"),
        P(None, "tp"),
        P(),
        P(),
        P("tp"),
        P(),
        P(),
    )
    out_specs = P(("grp", "dp"), ("sp", "tp"), None)


    return jax.shard_map(
        on_device, mesh=mesh, in_specs=in_specs, out_specs=out_specs, check_vma=False
    )
```

```python
import functools
import math

import jax
import jax.numpy as jnp
from jax import lax
from jax.experimental import pallas as pl
from jax.experimental.pallas import tpu as pltpu
from jax.sharding import PartitionSpec as P


HEADS = 8
HEAD_DIM = 128
GRID_WIDTH = 64
EPSILON = 1e-06
FACTOR = HEAD_DIM ** (-0.5)
LOG2E = math.log2(math.e)
F32 = jnp.float32
BF16 = jnp.bfloat16
MIB = 1 << 20


def local_call(body, outs, *, flops, limit=12, scratch=(), aliases=None, specs=None):
    single = not isinstance(outs, (tuple, list))
    shapes = [outs] if single else list(outs)
    space = pl.BlockSpec(memory_space=pltpu.VMEM)

    def run(*args):
        moved = sum(a.size * a.dtype.itemsize for a in args)
        moved += sum(math.prod(o.shape) * o.dtype.itemsize for o in shapes)
        return pl.pallas_call(
            body,
            out_shape=outs if single else tuple(shapes),
            in_specs=specs or [space] * len(args),
            out_specs=space if single else tuple([space] * len(shapes)),
            scratch_shapes=list(scratch),
            input_output_aliases=aliases or {},
            compiler_params=pltpu.CompilerParams(vmem_limit_bytes=limit * MIB),
            cost_estimate=pl.CostEstimate(
                flops=flops, bytes_accessed=moved, transcendentals=0
            ),
        )(*args)

    return run


FAR = pl.BlockSpec(memory_space=pltpu.MemorySpace.HBM)


def far(x):
    return pltpu.with_memory_space_constraint(x, pltpu.MemorySpace.HBM)


def shape(dims, dtype):
    return jax.ShapeDtypeStruct(dims, dtype)


def modulation_kernel(
    cond, cond_ctx, wa, wb, wc, out_ref, weights, own_ref, ctx_ref, rows_ref, sem
):
    copies = [
        pltpu.make_async_copy(source, target, sem.at[i])
        for i, (source, target) in enumerate(
            ((cond, own_ref), (cond_ctx, ctx_ref))
            + tuple((w, weights.at[i]) for i, w in enumerate((wa, wb, wc)))
        )
    ]
    for copy in copies:
        copy.start()
    copies.pop(0).wait()
    copies.pop(0).wait()
    depth = weights.shape[1]
    at = pl.ds(pl.multiple_of(lax.axis_index("sp") * depth, depth), depth)
    rows_ref[0:1, :] = own_ref[...].astype(F32)
    rows_ref[1:2, :] = ctx_ref[...].astype(F32).reshape(1, -1)
    rows = rows_ref[:, at]
    acted = (rows * jax.nn.sigmoid(rows)).astype(BF16)
    for copy in copies:
        copy.wait()
    shift, scale, gate = (
        jnp.dot(acted, weights[i], preferred_element_type=F32) for i in range(3)
    )
    mod = jnp.concatenate([shift[0:1], scale[0:1], shift[1:2], scale[1:2]], 0)
    part = gate.shape[1] // 4
    gate = jnp.concatenate([gate[0:1, i * part : (i + 1) * part] for i in range(4)], 0)
    mod = jnp.concatenate([mod, gate], 1)
    for i in range(out_ref.shape[0]):
        out_ref[i] = mod


def sum_kernel(parts, out_ref):
    out_ref[...] = jnp.sum(parts[...], 0)


def kv_kernel(
    owners, x0, x1, x2, x3, ctx, m0, m1, m2, m3, gain, wkv, key_gain, cosine, sine,
    chunk_ref, normed_ref, gate_ref, mod_ref,
):
    for i, mod in enumerate((m0, m1, m2, m3)):
        wide = gain.shape[1] // 4
        at = pl.ds(pl.multiple_of(owners[i] * wide, wide), wide)
        mod_ref[:, at] = mod[:, :wide]
        gate_ref[:, at] = jnp.concatenate([mod[r : r + 1, wide:] for r in range(4)], 1)

    def row_of(index):
        return mod_ref[index : index + 1, :]

    gains = gain[...]
    amp, shift = gains * (1.0 + row_of(1)), row_of(0)

    def norm(rows, amp, shift):
        rows = rows.astype(F32)
        mean = jnp.mean(rows * rows, -1, keepdims=True)
        return (rows * lax.rsqrt(mean + EPSILON) * amp + shift).astype(BF16)

    ctx_rows = ctx.shape[0]
    normed_ref[0:ctx_rows, :] = norm(ctx[...], gains * (1.0 + row_of(3)), row_of(2))
    own = x0.shape[0]
    for block, x in enumerate((x0, x1, x2, x3)):
        for t in range(own // 16):
            at = ctx_rows + block * own + t * 16
            normed_ref[at : at + 16, :] = norm(x[t * 16 : t * 16 + 16, :], amp, shift)
    kv = jnp.dot(normed_ref[...], wkv[...], preferred_element_type=F32)
    chunk_ref[1] = kv[:, HEAD_DIM:].astype(BF16)
    k = head_norm(kv[:, :HEAD_DIM], key_gain[...])
    chunk_ref[0, 0:ctx_rows, :] = k[0:ctx_rows].astype(BF16)
    chunk_ref[0, ctx_rows:, :] = rotate(k[ctx_rows:], cosine[...], sine[...]).astype(BF16)


def head_norm(vectors, gain):
    floats = vectors.astype(BF16).astype(F32)
    return floats * lax.rsqrt(jnp.mean(floats * floats, -1, keepdims=True) + EPSILON) * gain


def rotate(vectors, cosine, signed_sine):
    lanes = vectors.shape[-1]
    quarter = lanes // 4
    lane = lax.broadcasted_iota(jnp.int32, vectors.shape, 1)
    up = pltpu.roll(vectors, lanes - quarter, 1)
    down = pltpu.roll(vectors, quarter, 1)
    partner = jnp.where(lane % (2 * quarter) < quarter, up, down)
    return vectors * cosine + partner * signed_sine


def query_kernel(normed, wq, query_gain, cosine, sine, out_ref):
    rows = cosine.shape[0]
    skip = normed.shape[0] - rows
    q = jnp.dot(normed[skip:, :], wq[...], preferred_element_type=F32)
    for h in range(q.shape[1] // HEAD_DIM):
        one = head_norm(q[:, h * HEAD_DIM : (h + 1) * HEAD_DIM], query_gain[...])
        one = rotate(one, cosine[...], sine[...])
        out_ref[:, h * rows : (h + 1) * rows] = one.T.astype(BF16)


def attend_kernel(ctx_rows, first, pairs, *refs):
    refs = list(refs)
    qt, lift = refs[0], refs[1]
    if pairs:
        chunks = [(refs[2], refs[3])]
        rest = refs[4:]
    else:
        count = len(refs) - 2 - (2 if first else 4)
        chunks = [(r.at[0], r.at[1]) for r in refs[2 : 2 + count]]
        rest = refs[2 + count :]
    if first:
        acc_out, stat_out = rest
    else:
        acc_in, stat_in, acc_out, stat_out = rest
    total = qt.shape[1]
    width = 256


    @pl.loop(0, total // width)
    def _(block):
        part = pl.ds(pl.multiple_of(block * width, width), width)
        q = qt[:, part]
        bias = lift[:, part]
        if first:
            top = low = acc = None
        else:
            top, low, acc = stat_in[0:1, part], stat_in[1:2, part], acc_in[:, part]
        for k_ref, v_ref in chunks:
            s = jnp.dot(k_ref[...], q, preferred_element_type=F32)
            s = jnp.concatenate([s[:ctx_rows] + bias, s[ctx_rows:]], 0)
            new = jnp.max(s, 0, keepdims=True)
            if top is not None:
                new = jnp.maximum(top, new)
            p = jnp.exp2((s - new) * (FACTOR * LOG2E))
            size = jnp.sum(p, 0, keepdims=True)
            mixed = lax.dot_general(
                v_ref[...], p.astype(BF16), (((0,), (0,)), ((), ())), preferred_element_type=F32
            )
            if top is None:
                low, acc = size, mixed
            else:
                keep = jnp.exp2((top - new) * (FACTOR * LOG2E))
                low, acc = low * keep + size, acc * keep + mixed
            top = new
        acc_out[:, part] = acc
        stat_out[0:1, part] = top
        stat_out[1:2, part] = low


def keeping(body, source, *refs):
    *refs, kept, sem = refs
    load = pltpu.make_async_copy(source, kept, sem)
    load.start()
    body(*refs)
    load.wait()


def finish_kernel(acc, stat, *targets):
    own = targets[0].shape[0]
    rows = len(targets) * own
    for h in range(acc.shape[1] // rows):
        part = slice(h * rows, (h + 1) * rows)
        att = (acc[:, part] / stat[1:2, part]).T.astype(BF16)
        for b, target in enumerate(targets):
            target[:, h * HEAD_DIM : (h + 1) * HEAD_DIM] = att[b * own : (b + 1) * own]


def out_kernel(order, a0, a1, a2, a3, gain, w_out, latent, gate, out_ref):
    wide = 512
    cols = a0.shape[1]
    atts = [a[...].astype(F32) for a in (a0, a1, a2, a3)]
    total = sum(jnp.sum(a * a, -1, keepdims=True) for a in atts)
    scale = lax.rsqrt(total / (cols * len(atts)) + EPSILON)
    normed = [
        (a * scale * gain[pl.ds(order[i], 1), :]).astype(BF16) for i, a in enumerate(atts)
    ]
    for begin in range(0, out_ref.shape[1], wide):
        part = slice(begin, begin + wide)
        mix = 0.0
        for i, a in enumerate(normed):
            at = pl.multiple_of(order[i] * cols, cols)
            mix += jnp.dot(a, w_out[pl.ds(at, cols), part], preferred_element_type=F32)
        out = latent[:, part].astype(F32) + gate[:, part] * mix
        out_ref[:, part] = out.astype(BF16)


def angles(positions):
    freqs = HEAD_DIM // 4
    rows = (positions // GRID_WIDTH).astype(F32)
    cols = (positions % GRID_WIDTH).astype(F32)
    inverse = 10000.0 ** (-jnp.arange(freqs, dtype=F32) / freqs)
    by_row, by_col = rows[:, None] * inverse, cols[:, None] * inverse
    cosine = [jnp.cos(by_row)] * 2 + [jnp.cos(by_col)] * 2
    sine = [-jnp.sin(by_row), jnp.sin(by_row), -jnp.sin(by_col), jnp.sin(by_col)]
    return jnp.concatenate(cosine, 1), jnp.concatenate(sine, 1)


def shifted(x, axis, by):
    count = lax.axis_size(axis)
    return lax.ppermute(x, axis, [(i, (i + by) % count) for i in range(count)])


def on_device(
    latent,
    cond,
    context,
    cond_ctx,
    w_shift,
    w_scale,
    w_gate,
    norm_gain,
    w_query,
    w_key,
    w_value,
    query_gain,
    key_gain,
    ctx_lift,
    out_gain,
    w_out,
):
    sp, tp = lax.axis_index("sp"), lax.axis_index("tp")
    n_sp, n_tp = lax.axis_size("sp"), lax.axis_size("tp")
    own_rows, width = latent.shape[1:]
    latent, context = latent[0], context[0]
    ctx_rows = context.shape[0]
    rows = own_rows * n_tp
    in_rows, out_cols = w_shift.shape

    space = pl.BlockSpec(memory_space=pltpu.VMEM)
    packed = (4, out_cols + out_cols // 4)
    parts = pl.pallas_call(
        modulation_kernel,
        out_shape=shape((n_sp, *packed), F32),
        in_specs=[FAR] * 5,
        out_specs=space,
        scratch_shapes=[
            pltpu.VMEM((3, in_rows, out_cols), BF16),
            pltpu.VMEM((1, width), BF16),
            pltpu.VMEM((width,), BF16),
            pltpu.VMEM((2, width), F32),
            pltpu.SemaphoreType.DMA((5,)),
        ],
        compiler_params=pltpu.CompilerParams(vmem_limit_bytes=4 * MIB),
        cost_estimate=pl.CostEstimate(flops=10**6, bytes_accessed=MIB, transcendentals=0),
        name="modulation",
    )(far(cond), far(cond_ctx), far(w_shift), far(w_scale), far(w_gate))
    parts = lax.all_to_all(parts, "sp", 0, 0)
    summed = local_call(sum_kernel, shape(packed, F32), flops=10**6, limit=4)(parts)
    mods = [summed] + [shifted(summed, "tp", by) for by in (1, -1, 2)]

    latents = [latent]
    for by in (1, -1, 2):
        latents.append(shifted(latent, "tp", by))
    owners = jnp.stack([tp, (tp - 1) % n_tp, (tp + 1) % n_tp, (tp + 2) % n_tp]).astype(jnp.int32)
    positions = sp * rows + (owners[:, None] * own_rows + jnp.arange(own_rows)[None]).reshape(-1)
    cosine, sine = angles(positions.astype(jnp.int32))
    wkv = jnp.concatenate([w_key, w_value], 1)
    length = ctx_rows + rows
    chunk, normed, gate = local_call(
        kv_kernel,
        (
            shape((2, length, HEAD_DIM), BF16),
            shape((length, width), BF16),
            shape((1, width), F32),
        ),
        flops=2 * length * width * 256,
        limit=16,
        specs=[pl.BlockSpec(memory_space=pltpu.SMEM)] + [space] * 14,
        scratch=[pltpu.VMEM((4, width), F32)],
    )(owners, *latents, context, *mods, norm_gain[None], wkv, key_gain[None], cosine, sine)
    q_cols = w_query.shape[1]
    group = q_cols // HEAD_DIM
    qt = local_call(
        query_kernel, shape((HEAD_DIM, group * rows), BF16), flops=2 * rows * width * q_cols, limit=16
    )(normed, w_query, query_gain[None], cosine, sine)
    lift = (ctx_lift + math.log(rows / ctx_rows)) / FACTOR
    lift = jnp.repeat(lift, rows)[None]

    order = jnp.stack([tp, (tp + 1) % n_tp, (tp - 1) % n_tp, (tp + 2) % n_tp]).astype(jnp.int32)
    gain_rows = out_gain.reshape(n_tp, q_cols)
    order, gain_rows, lift, chunk = lax.optimization_barrier((order, gain_rows, lift, chunk))

    lanes = group * rows
    state_shapes = (shape((HEAD_DIM, lanes), F32), shape((2, lanes), F32))
    state = local_call(
        functools.partial(attend_kernel, ctx_rows, True, False),
        state_shapes,
        flops=4 * length * lanes * HEAD_DIM,
    )(qt, lift, chunk)

    def attend(state, *chunks, pairs=False):
        count = 1 if pairs else len(chunks)
        given = (qt, lift, *chunks, *state)
        return local_call(
            functools.partial(attend_kernel, ctx_rows, False, pairs),
            state_shapes,
            flops=4 * count * length * lanes * HEAD_DIM,
            aliases={len(given) - 2: 0, len(given) - 1: 1},
        )(*given)

    def hop(x, by, state):
        x, state = lax.optimization_barrier((x, state))
        return x, shifted(x, "sp", by), state

    right, left = shifted(chunk, "sp", 1), shifted(chunk, "sp", -1)
    for _ in range(n_sp // 2 - 2):
        here_right, right, state = hop(right, 1, state)
        here_left, left, state = hop(left, -1, state)
        state = attend(state, here_right, here_left)
    right, state = lax.optimization_barrier((right, state))
    last_k = shifted(right[0], "sp", 1)
    left, state = lax.optimization_barrier((left, state))
    last_v = shifted(left[1], "sp", -1)
    *state, w_kept = local_call(
        functools.partial(keeping, functools.partial(attend_kernel, ctx_rows, False, False)),
        (*state_shapes, pltpu.VMEM(w_out.shape, BF16)),
        flops=8 * length * lanes * HEAD_DIM,
        specs=[FAR] + [space] * 6,
        scratch=[pltpu.SemaphoreType.DMA],
        aliases={5: 0, 6: 1},
    )(far(w_out), qt, lift, right, left, *state)
    state = attend(state, last_k, last_v, pairs=True)

    own, to_left, to_right, to_far = local_call(
        finish_kernel, [shape((own_rows, q_cols), BF16)] * n_tp, flops=10**6
    )(*state)
    atts = [own, shifted(to_left, "tp", -1), shifted(to_right, "tp", 1), shifted(to_far, "tp", 2)]
    result = local_call(
        out_kernel,
        shape((own_rows, width), BF16),
        flops=2 * own_rows * width * HEADS * HEAD_DIM,
        specs=[pl.BlockSpec(memory_space=pltpu.SMEM)] + [space] * 8,
    )(order, *atts, gain_rows, w_kept, latent, gate)
    return result[None]


def solution(mesh):
    in_specs = (
        P(("grp", "dp"), ("sp", "tp"), None),
        P(("grp", "dp"), None),
        P(("grp", "dp"), "sp", None),
        P(),
        P("sp", "tp"),
        P("sp", "tp"),
        P("sp", "tp"),
        P(),
        P(None, "tp"),
        P(None, "tp"),
        P(None, "tp"),
        P(),
        P(),
        P("tp"),
        P(),
        P(),
    )
    out_specs = P(("grp", "dp"), ("sp", "tp"), None)


    return jax.shard_map(
        on_device, mesh=mesh, in_specs=in_specs, out_specs=out_specs, check_vma=False
    )
```

```python
import functools
import math

import jax
import jax.numpy as jnp
from jax import lax
from jax.experimental import pallas as pl
from jax.experimental.pallas import tpu as pltpu
from jax.sharding import PartitionSpec as P


HEADS = 8
HEAD_DIM = 128
GRID_WIDTH = 64
EPSILON = 1e-06
FACTOR = HEAD_DIM ** (-0.5)
LOG2E = math.log2(math.e)
F32 = jnp.float32
BF16 = jnp.bfloat16
MIB = 1 << 20


def local_call(body, outs, *, flops, limit=12, scratch=(), aliases=None, specs=None):
    single = not isinstance(outs, (tuple, list))
    shapes = [outs] if single else list(outs)
    space = pl.BlockSpec(memory_space=pltpu.VMEM)

    def run(*args):
        moved = sum(a.size * a.dtype.itemsize for a in args)
        moved += sum(math.prod(o.shape) * o.dtype.itemsize for o in shapes)
        return pl.pallas_call(
            body,
            out_shape=outs if single else tuple(shapes),
            in_specs=specs or [space] * len(args),
            out_specs=space if single else tuple([space] * len(shapes)),
            scratch_shapes=list(scratch),
            input_output_aliases=aliases or {},
            compiler_params=pltpu.CompilerParams(vmem_limit_bytes=limit * MIB),
            cost_estimate=pl.CostEstimate(
                flops=flops, bytes_accessed=moved, transcendentals=0
            ),
        )(*args)

    return run


FAR = pl.BlockSpec(memory_space=pltpu.MemorySpace.HBM)


def far(x):
    return pltpu.with_memory_space_constraint(x, pltpu.MemorySpace.HBM)


def shape(dims, dtype):
    return jax.ShapeDtypeStruct(dims, dtype)


def modulation_kernel(
    cond, cond_ctx, wa, wb, wc, out_ref, weights, own_ref, ctx_ref, rows_ref, sem
):
    copies = [
        pltpu.make_async_copy(source, target, sem.at[i])
        for i, (source, target) in enumerate(
            ((cond, own_ref), (cond_ctx, ctx_ref))
            + tuple((w, weights.at[i]) for i, w in enumerate((wa, wb, wc)))
        )
    ]
    for copy in copies:
        copy.start()
    copies.pop(0).wait()
    copies.pop(0).wait()
    depth = weights.shape[1]
    at = pl.ds(pl.multiple_of(lax.axis_index("sp") * depth, depth), depth)
    rows_ref[0:1, :] = own_ref[...].astype(F32)
    rows_ref[1:2, :] = ctx_ref[...].astype(F32).reshape(1, -1)
    rows = rows_ref[:, at]
    acted = (rows * jax.nn.sigmoid(rows)).astype(BF16)
    for copy in copies:
        copy.wait()
    shift, scale, gate = (
        jnp.dot(acted, weights[i], preferred_element_type=F32) for i in range(3)
    )
    mod = jnp.concatenate([shift[0:1], scale[0:1], shift[1:2], scale[1:2]], 0)
    part = gate.shape[1] // 4
    gate = jnp.concatenate([gate[0:1, i * part : (i + 1) * part] for i in range(4)], 0)
    mod = jnp.concatenate([mod, gate], 1)
    for i in range(out_ref.shape[0]):
        out_ref[i] = mod


def sum_kernel(parts, out_ref):
    out_ref[...] = jnp.sum(parts[...], 0)


def kv_kernel(
    owners, x0, x1, x2, x3, ctx, m0, m1, m2, m3, gain, wkv, key_gain, cosine, sine,
    chunk_ref, normed_ref, gate_ref, mod_ref,
):
    for i, mod in enumerate((m0, m1, m2, m3)):
        wide = gain.shape[1] // 4
        at = pl.ds(pl.multiple_of(owners[i] * wide, wide), wide)
        mod_ref[:, at] = mod[:, :wide]
        gate_ref[:, at] = jnp.concatenate([mod[r : r + 1, wide:] for r in range(4)], 1)

    def row_of(index):
        return mod_ref[index : index + 1, :]

    gains = gain[...]
    amp, shift = gains * (1.0 + row_of(1)), row_of(0)

    def norm(rows, amp, shift):
        rows = rows.astype(F32)
        mean = jnp.mean(rows * rows, -1, keepdims=True)
        return (rows * lax.rsqrt(mean + EPSILON) * amp + shift).astype(BF16)

    ctx_rows = ctx.shape[0]
    normed_ref[0:ctx_rows, :] = norm(ctx[...], gains * (1.0 + row_of(3)), row_of(2))
    own = x0.shape[0]
    for block, x in enumerate((x0, x1, x2, x3)):
        for t in range(own // 16):
            at = ctx_rows + block * own + t * 16
            normed_ref[at : at + 16, :] = norm(x[t * 16 : t * 16 + 16, :], amp, shift)
    kv = jnp.dot(normed_ref[...], wkv[...], preferred_element_type=F32)
    chunk_ref[1] = kv[:, HEAD_DIM:].astype(BF16)
    k = head_norm(kv[:, :HEAD_DIM], key_gain[...])
    chunk_ref[0, 0:ctx_rows, :] = k[0:ctx_rows].astype(BF16)
    chunk_ref[0, ctx_rows:, :] = rotate(k[ctx_rows:], cosine[...], sine[...]).astype(BF16)


def head_norm(vectors, gain):
    floats = vectors.astype(BF16).astype(F32)
    return floats * lax.rsqrt(jnp.mean(floats * floats, -1, keepdims=True) + EPSILON) * gain


def rotate(vectors, cosine, signed_sine):
    lanes = vectors.shape[-1]
    quarter = lanes // 4
    lane = lax.broadcasted_iota(jnp.int32, vectors.shape, 1)
    up = pltpu.roll(vectors, lanes - quarter, 1)
    down = pltpu.roll(vectors, quarter, 1)
    partner = jnp.where(lane % (2 * quarter) < quarter, up, down)
    return vectors * cosine + partner * signed_sine


def query_kernel(normed, wq, query_gain, cosine, sine, out_ref):
    rows = cosine.shape[0]
    skip = normed.shape[0] - rows
    q = jnp.dot(normed[skip:, :], wq[...], preferred_element_type=F32)
    for h in range(q.shape[1] // HEAD_DIM):
        one = head_norm(q[:, h * HEAD_DIM : (h + 1) * HEAD_DIM], query_gain[...])
        one = rotate(one, cosine[...], sine[...])
        out_ref[:, h * rows : (h + 1) * rows] = one.T.astype(BF16)


def attend_kernel(ctx_rows, first, *refs):
    qt, lift, *refs = refs
    if first:
        *refs, acc_out, stat_out = refs
    else:
        *refs, acc_in, stat_in, acc_out, stat_out = refs
    chunks = [(r.at[0], r.at[1]) for r in refs]
    total = qt.shape[1]
    width = 256


    @pl.loop(0, total // width)
    def _(block):
        part = pl.ds(pl.multiple_of(block * width, width), width)
        q = qt[:, part]
        bias = lift[:, part]
        if first:
            top = low = acc = None
        else:
            top, low, acc = stat_in[0:1, part], stat_in[1:2, part], acc_in[:, part]
        for k_ref, v_ref in chunks:
            s = jnp.dot(k_ref[...], q, preferred_element_type=F32)
            s = jnp.concatenate([s[:ctx_rows] + bias, s[ctx_rows:]], 0)
            new = jnp.max(s, 0, keepdims=True)
            if top is not None:
                new = jnp.maximum(top, new)
            p = jnp.exp2((s - new) * (FACTOR * LOG2E))
            size = jnp.sum(p, 0, keepdims=True)
            mixed = lax.dot_general(
                v_ref[...], p.astype(BF16), (((0,), (0,)), ((), ())), preferred_element_type=F32
            )
            if top is None:
                low, acc = size, mixed
            else:
                keep = jnp.exp2((top - new) * (FACTOR * LOG2E))
                low, acc = low * keep + size, acc * keep + mixed
            top = new
        acc_out[:, part] = acc
        stat_out[0:1, part] = top
        stat_out[1:2, part] = low


def keeping(body, source, *refs):
    *refs, kept, sem = refs
    load = pltpu.make_async_copy(source, kept, sem)
    load.start()
    body(*refs)
    load.wait()


def finish_kernel(acc, stat, *targets):
    own = targets[0].shape[0]
    rows = len(targets) * own
    for h in range(acc.shape[1] // rows):
        part = slice(h * rows, (h + 1) * rows)
        att = (acc[:, part] / stat[1:2, part]).T.astype(BF16)
        for b, target in enumerate(targets):
            target[:, h * HEAD_DIM : (h + 1) * HEAD_DIM] = att[b * own : (b + 1) * own]


def out_kernel(order, a0, a1, a2, a3, gain, w_out, latent, gate, out_ref):
    wide = 512
    cols = a0.shape[1]
    atts = [a[...].astype(F32) for a in (a0, a1, a2, a3)]
    total = sum(jnp.sum(a * a, -1, keepdims=True) for a in atts)
    scale = lax.rsqrt(total / (cols * len(atts)) + EPSILON)
    normed = [
        (a * scale * gain[pl.ds(order[i], 1), :]).astype(BF16) for i, a in enumerate(atts)
    ]
    for begin in range(0, out_ref.shape[1], wide):
        part = slice(begin, begin + wide)
        mix = 0.0
        for i, a in enumerate(normed):
            at = pl.multiple_of(order[i] * cols, cols)
            mix += jnp.dot(a, w_out[pl.ds(at, cols), part], preferred_element_type=F32)
        out = latent[:, part].astype(F32) + gate[:, part] * mix
        out_ref[:, part] = out.astype(BF16)


def angles(positions):
    freqs = HEAD_DIM // 4
    rows = (positions // GRID_WIDTH).astype(F32)
    cols = (positions % GRID_WIDTH).astype(F32)
    inverse = 10000.0 ** (-jnp.arange(freqs, dtype=F32) / freqs)
    by_row, by_col = rows[:, None] * inverse, cols[:, None] * inverse
    cosine = [jnp.cos(by_row)] * 2 + [jnp.cos(by_col)] * 2
    sine = [-jnp.sin(by_row), jnp.sin(by_row), -jnp.sin(by_col), jnp.sin(by_col)]
    return jnp.concatenate(cosine, 1), jnp.concatenate(sine, 1)


def shifted(x, axis, by):
    count = lax.axis_size(axis)
    return lax.ppermute(x, axis, [(i, (i + by) % count) for i in range(count)])


def on_device(
    latent,
    cond,
    context,
    cond_ctx,
    w_shift,
    w_scale,
    w_gate,
    norm_gain,
    w_query,
    w_key,
    w_value,
    query_gain,
    key_gain,
    ctx_lift,
    out_gain,
    w_out,
):
    sp, tp = lax.axis_index("sp"), lax.axis_index("tp")
    n_sp, n_tp = lax.axis_size("sp"), lax.axis_size("tp")
    own_rows, width = latent.shape[1:]
    latent, context = latent[0], context[0]
    ctx_rows = context.shape[0]
    rows = own_rows * n_tp
    in_rows, out_cols = w_shift.shape

    space = pl.BlockSpec(memory_space=pltpu.VMEM)
    packed = (4, out_cols + out_cols // 4)
    parts = pl.pallas_call(
        modulation_kernel,
        out_shape=shape((n_sp, *packed), F32),
        in_specs=[FAR] * 5,
        out_specs=space,
        scratch_shapes=[
            pltpu.VMEM((3, in_rows, out_cols), BF16),
            pltpu.VMEM((1, width), BF16),
            pltpu.VMEM((width,), BF16),
            pltpu.VMEM((2, width), F32),
            pltpu.SemaphoreType.DMA((5,)),
        ],
        compiler_params=pltpu.CompilerParams(vmem_limit_bytes=4 * MIB),
        cost_estimate=pl.CostEstimate(flops=10**6, bytes_accessed=MIB, transcendentals=0),
        name="modulation",
    )(far(cond), far(cond_ctx), far(w_shift), far(w_scale), far(w_gate))
    parts = lax.all_to_all(parts, "sp", 0, 0)
    summed = local_call(sum_kernel, shape(packed, F32), flops=10**6, limit=4)(parts)
    mods = [summed] + [shifted(summed, "tp", by) for by in (1, -1, 2)]

    latents = [latent]
    for by in (1, -1, 2):
        latents.append(shifted(latent, "tp", by))
    owners = jnp.stack([tp, (tp - 1) % n_tp, (tp + 1) % n_tp, (tp + 2) % n_tp]).astype(jnp.int32)
    positions = sp * rows + (owners[:, None] * own_rows + jnp.arange(own_rows)[None]).reshape(-1)
    cosine, sine = angles(positions.astype(jnp.int32))
    wkv = jnp.concatenate([w_key, w_value], 1)
    length = ctx_rows + rows
    chunk, normed, gate = local_call(
        kv_kernel,
        (
            shape((2, length, HEAD_DIM), BF16),
            shape((length, width), BF16),
            shape((1, width), F32),
        ),
        flops=2 * length * width * 256,
        limit=16,
        specs=[pl.BlockSpec(memory_space=pltpu.SMEM)] + [space] * 14,
        scratch=[pltpu.VMEM((4, width), F32)],
    )(owners, *latents, context, *mods, norm_gain[None], wkv, key_gain[None], cosine, sine)
    q_cols = w_query.shape[1]
    group = q_cols // HEAD_DIM
    qt = local_call(
        query_kernel, shape((HEAD_DIM, group * rows), BF16), flops=2 * rows * width * q_cols, limit=16
    )(normed, w_query, query_gain[None], cosine, sine)
    lift = (ctx_lift + math.log(rows / ctx_rows)) / FACTOR
    lift = jnp.repeat(lift, rows)[None]

    order = jnp.stack([tp, (tp + 1) % n_tp, (tp - 1) % n_tp, (tp + 2) % n_tp]).astype(jnp.int32)
    gain_rows = out_gain.reshape(n_tp, q_cols)
    order, gain_rows, lift, chunk = lax.optimization_barrier((order, gain_rows, lift, chunk))

    lanes = group * rows
    state_shapes = (shape((HEAD_DIM, lanes), F32), shape((2, lanes), F32))
    state = local_call(
        functools.partial(attend_kernel, ctx_rows, True),
        state_shapes,
        flops=4 * length * lanes * HEAD_DIM,
    )(qt, lift, chunk)

    def attend(state, *chunks):
        given = (qt, lift, *chunks, *state)
        return local_call(
            functools.partial(attend_kernel, ctx_rows, False),
            state_shapes,
            flops=4 * len(chunks) * length * lanes * HEAD_DIM,
            aliases={len(given) - 2: 0, len(given) - 1: 1},
        )(*given)

    def hop(x, by, state):
        x, state = lax.optimization_barrier((x, state))
        return x, shifted(x, "sp", by), state

    right, left = shifted(chunk, "sp", 1), shifted(chunk, "sp", -1)
    for _ in range(n_sp // 2 - 2):
        here_right, right, state = hop(right, 1, state)
        here_left, left, state = hop(left, -1, state)
        state = attend(state, here_right, here_left)
    right, last, state = hop(right, 1, state)
    *state, w_kept = local_call(
        functools.partial(keeping, functools.partial(attend_kernel, ctx_rows, False)),
        (*state_shapes, pltpu.VMEM(w_out.shape, BF16)),
        flops=8 * length * lanes * HEAD_DIM,
        specs=[FAR] + [space] * 6,
        scratch=[pltpu.SemaphoreType.DMA],
        aliases={5: 0, 6: 1},
    )(far(w_out), qt, lift, right, left, *state)
    state = attend(state, last)

    own, to_left, to_right, to_far = local_call(
        finish_kernel, [shape((own_rows, q_cols), BF16)] * n_tp, flops=10**6
    )(*state)
    atts = [own, shifted(to_left, "tp", -1), shifted(to_right, "tp", 1), shifted(to_far, "tp", 2)]
    result = local_call(
        out_kernel,
        shape((own_rows, width), BF16),
        flops=2 * own_rows * width * HEADS * HEAD_DIM,
        specs=[pl.BlockSpec(memory_space=pltpu.SMEM)] + [space] * 8,
    )(order, *atts, gain_rows, w_kept, latent, gate)
    return result[None]


def solution(mesh):
    in_specs = (
        P(("grp", "dp"), ("sp", "tp"), None),
        P(("grp", "dp"), None),
        P(("grp", "dp"), "sp", None),
        P(),
        P("sp", "tp"),
        P("sp", "tp"),
        P("sp", "tp"),
        P(),
        P(None, "tp"),
        P(None, "tp"),
        P(None, "tp"),
        P(),
        P(),
        P("tp"),
        P(),
        P(),
    )
    out_specs = P(("grp", "dp"), ("sp", "tp"), None)


    return jax.shard_map(
        on_device, mesh=mesh, in_specs=in_specs, out_specs=out_specs, check_vma=False
    )
```
